32 devices in a mesh: sp: 4 (over z), fs: 4 (over y, x), tp: 2 (over core).
Axes of the slice: x: 2, y: 2, z: 4, core: 2. Of those that a mesh axis runs over, the one named last changes fastest.
Arguments:
- tokens: bfloat16 [4096, 2048], P(('fs', 'sp')), parts along dimension 0, may hold values from -6 to 6
- norm_gain: float32 [2048], replicated, may hold values from 0.1 to 1.9
- w_query: bfloat16 [2048, 1024], P('sp', 'tp'), may hold values from -0.080939698 to 0.080939698
- w_key: bfloat16 [2048, 256], P('sp', 'tp'), may hold values from -0.080939698 to 0.080939698
- w_value: bfloat16 [2048, 256], P('sp', 'tp'), may hold values from -0.125 to 0.125
- w_conv_in: bfloat16 [2048, 1024], P('sp', 'tp'), may hold values from -0.125 to 0.125
- w_conv_gate: bfloat16 [2048, 1024], P('sp', 'tp'), may hold values from -0.125 to 0.125
- sink_logit: float32 [16], P('tp'), may hold values from 2 to 6
- conv_taps: float32 [31, 1024], P(None, 'tp'), may hold values from -5.3881591 to 5.3881591
- conv_bias: float32 [1024], P('tp'), may hold values from -0.9 to 5.9
- channel_gain: float32 [1024], P('tp'), may hold values from 0.1 to 1.9
- channel_shift: float32 [1024], P('tp'), may hold values from -3 to 3
- w_attn_out: bfloat16 [1024, 2048], P(None, 'sp'), may hold values from -1.5 to 1.5
- w_conv_out: bfloat16 [1024, 2048], P(None, 'sp'), may hold values from -0.1875 to 0.1875
Outputs:
- output: bfloat16 [4096, 2048], P(('fs', 'sp', 'tp')), parts along dimension 0
The draws below stay inside these ranges and needn't reach their ends.
There are 4 independent parts, one for each index of `fs`. The reference program is written for one: setup_inputs(seed, part) draws one part's arguments, and reference() takes and returns one part's arrays. A program takes and returns all parts, laid end to end along the dimension named above; an argument that names none is the same for every part. Nothing has to cross between parts.
All inputs are finite; a program needn't handle non-finite values.
Results may differ from the reference program's by a relative error of at most 0.011.
Values may be sent and summed in bfloat16 or wider, within the bound.
No kernel may reach another device: no remote copies, remote signals or barrier semaphores. Data moves between devices by JAX's collectives and lax.ppermute only.
A program may use at most 64 MiB of HBM per device.

```python
import jax
import jax.numpy as jnp
from jax import lax

D = 2048
HEADS = 16
KV_HEADS = 4
HEAD_DIM = 64
CHANNELS = 1024
TAPS = 31
WINDOW = 128
GRID_W = 64
TOK_DEV = 256
SEQ = 1024
ATT_WIDTH = 1024
KV_WIDTH = 256


def draw_tokens(key, part):
    noise_key = jax.random.fold_in(key, 0)
    result = jnp.clip(jax.random.normal(noise_key, (SEQ, D), jnp.float32), -6.0, 6.0)
    return result.astype(jnp.bfloat16)


def draw_w_query(key, part):
    base = jnp.clip(jax.random.normal(jax.random.fold_in(key, 11), (D, HEADS * HEAD_DIM), jnp.float32), -3.0, 3.0) * D ** (-0.5)
    return base.astype(jnp.bfloat16)


def draw_w_key(key, part):
    base = jnp.clip(jax.random.normal(jax.random.fold_in(key, 12), (D, KV_HEADS * HEAD_DIM), jnp.float32), -3.0, 3.0) * D ** (-0.5)
    return base.astype(jnp.bfloat16)


def draw_conv_taps(key, part):
    base_key, jitter_key = jax.random.split(jax.random.fold_in(key, 13))
    base = jnp.clip(jax.random.normal(base_key, (TAPS, CHANNELS), jnp.float32), -3.0, 3.0)
    order = jnp.arange(CHANNELS, dtype=jnp.float32) / CHANNELS
    jitter = jnp.clip(jax.random.normal(jitter_key, (CHANNELS,), jnp.float32), -3.0, 3.0)
    exponent = jnp.clip(order + 0.15 * jitter, 0.0, 1.0)
    return (base * TAPS ** (-0.5) * 10.0 ** exponent[None, :]).astype(jnp.float32)


def draw_conv_bias(key, part):
    order = jnp.arange(CHANNELS, dtype=jnp.float32) / CHANNELS
    jitter = jnp.clip(jax.random.normal(jax.random.fold_in(key, 14), (CHANNELS,), jnp.float32), -3.0, 3.0)
    ramp = 3.0 * order
    return (ramp + 0.3 * jitter).astype(jnp.float32)


def levels(rng, shape, pieces, smallest, largest):
    factor_of = 1.0
    for axis_at, shards_of in pieces:
        draws = jax.random.uniform(jax.random.fold_in(jax.random.fold_in(rng, 6), axis_at), (shards_of,), jnp.float32, smallest / len(pieces), largest / len(pieces))
        factor_of = factor_of * jnp.repeat(jnp.exp(draws), shape[axis_at] // shards_of).reshape((-1,) + (1,) * (len(shape) - 1 - axis_at))
    return factor_of


def normal_values(key, shape, deviation, limit, cuts=(), held_as=jnp.bfloat16):
    array = deviation * jax.random.normal(key, shape, jnp.float32)
    if cuts:
        array = array * levels(key, shape, cuts, -0.22, 0.18)
    return jnp.clip(array, -limit, limit).astype(held_as)


def setup_inputs(seed: int = 0, part: int = 0) -> dict:
    arg_keys = jax.random.split(jax.random.key(seed), 15)
    part_keys = jax.random.split(jax.random.fold_in(arg_keys[14], part), 15)
    tokens = draw_tokens(jax.random.fold_in(jax.random.fold_in(arg_keys[14], part), 71), part)
    norm_gain = jnp.clip(1.0 + 0.18 * jax.random.normal(arg_keys[1], (D,), jnp.float32), 0.1, 1.9)
    w_query = draw_w_query(jax.random.fold_in(arg_keys[14], 71), part)
    w_key = draw_w_key(jax.random.fold_in(arg_keys[14], 71), part)
    w_value = normal_values(arg_keys[4], (D, KV_WIDTH), D ** -0.5, 0.125, ((0, 4), (1, 2)))
    w_conv_in = normal_values(arg_keys[5], (D, CHANNELS), D ** -0.5, 0.125, ((0, 4), (1, 2)))
    w_conv_gate = normal_values(arg_keys[6], (D, CHANNELS), D ** -0.5, 0.125, ((0, 4), (1, 2)))
    sink_logit = jnp.clip(2.0 + 4.0 * jax.random.uniform(arg_keys[7], (HEADS,), jnp.float32) ** levels(arg_keys[7], (HEADS,), ((0, 2),), -0.2, 0.2), 2.0, 6.0)
    conv_taps = draw_conv_taps(jax.random.fold_in(arg_keys[14], 71), part)
    conv_bias = draw_conv_bias(jax.random.fold_in(arg_keys[14], 71), part)
    channel_gain = jnp.clip(1.0 + 0.18 * jax.random.normal(arg_keys[10], (CHANNELS,), jnp.float32), 0.1, 1.9)
    channel_shift = normal_values(arg_keys[11], (CHANNELS,), 0.5, 3.0, ((0, 2),), jnp.float32)
    w_attn_out = normal_values(arg_keys[12], (ATT_WIDTH, D), (max(ATT_WIDTH // 64, 1)) ** -0.5, 1.5, ((1, 4),))
    w_conv_out = normal_values(arg_keys[13], (CHANNELS, D), CHANNELS ** -0.5, 0.1875, ((1, 4),))
    return {"tokens": tokens, "norm_gain": norm_gain, "w_query": w_query, "w_key": w_key, "w_value": w_value, "w_conv_in": w_conv_in, "w_conv_gate": w_conv_gate, "sink_logit": sink_logit, "conv_taps": conv_taps, "conv_bias": conv_bias, "channel_gain": channel_gain, "channel_shift": channel_shift, "w_attn_out": w_attn_out, "w_conv_out": w_conv_out}


EPSILON = 1e-06
NEGATIVE = -1e+30
ROPE_BASE = 10000.0

def rotate_pairs(values, positions):
    middle = values.shape[-1] // 2
    inverse = ROPE_BASE ** (-jnp.arange(middle, dtype=jnp.float32) / middle)
    angles = positions.astype(jnp.float32)[:, None] * inverse[None, :]
    cosine = jnp.cos(angles)[:, None, :]
    sine_table = jnp.sin(angles)[:, None, :]
    leading = values[..., :middle]
    trailing = values[..., middle:]
    return jnp.concatenate([leading * cosine - trailing * sine_table, leading * sine_table + trailing * cosine], axis=-1)

def grid_rotate(values, positions):
    middle = values.shape[-1] // 2
    return jnp.concatenate([rotate_pairs(values[..., :middle], positions // GRID_W), rotate_pairs(values[..., middle:], positions % GRID_W)], axis=-1)

def reference(tokens, norm_gain, w_query, w_key, w_value, w_conv_in, w_conv_gate, sink_logit, conv_taps, conv_bias, channel_gain, channel_shift, w_attn_out, w_conv_out):
    total = tokens.shape[0]
    token_float = tokens.astype(jnp.float32)
    normed = (token_float * lax.rsqrt(lax.optimization_barrier(jnp.mean(token_float * token_float, axis=-1, keepdims=True)) + EPSILON) * norm_gain[None, :]).astype(jnp.bfloat16)
    positions = jnp.arange(total, dtype=jnp.int32)
    group = HEADS // KV_HEADS
    query = jnp.dot(normed, w_query, preferred_element_type=jnp.float32).reshape(total, HEADS, HEAD_DIM)
    query = grid_rotate(query, positions).astype(jnp.bfloat16)
    keys = jnp.dot(normed, w_key, preferred_element_type=jnp.float32).reshape(total, KV_HEADS, HEAD_DIM)
    keys = grid_rotate(keys, positions).astype(jnp.bfloat16)
    values = jnp.dot(normed, w_value, preferred_element_type=jnp.float32).astype(jnp.bfloat16)
    values = values.reshape(total, KV_HEADS, HEAD_DIM)
    padded_keys = jnp.pad(keys, ((WINDOW, WINDOW), (0, 0), (0, 0)))
    padded_values = jnp.pad(values, ((WINDOW, WINDOW), (0, 0), (0, 0)))
    block = min(TOK_DEV, 512)
    span = block + 2 * WINDOW
    sinks = sink_logit.astype(jnp.float32).reshape(KV_HEADS, group)[:, :, None, None]

    def attend(block_index):
        start = (block_index * block).astype(jnp.int32)
        queries = lax.dynamic_slice_in_dim(query, start, block, 0).reshape(block, KV_HEADS, group, HEAD_DIM)
        near_keys = lax.dynamic_slice_in_dim(padded_keys, start, span, 0)
        near_values = lax.dynamic_slice_in_dim(padded_values, start, span, 0)
        scores = jnp.einsum('qkgd,skd->kgqs', queries.astype(jnp.float32), near_keys.astype(jnp.float32)) * HEAD_DIM ** (-0.5)
        query_pos = start + jnp.arange(block, dtype=jnp.int32)
        key_pos = start - WINDOW + jnp.arange(span, dtype=jnp.int32)
        valid = (jnp.abs(query_pos[:, None] - key_pos[None, :]) <= WINDOW) & (key_pos[None, :] >= 0) & (key_pos[None, :] < total)
        scores = jnp.where(valid[None, None], scores, NEGATIVE)
        top = jnp.maximum(lax.optimization_barrier(jnp.max(scores, axis=-1, keepdims=True)), sinks)
        raised = jnp.exp(scores - top)
        denominator = lax.optimization_barrier(jnp.sum(raised, axis=-1, keepdims=True)) + jnp.exp(sinks - top)
        probs = (raised / denominator).astype(jnp.bfloat16)
        mixed = jnp.einsum('kgqs,skd->qkgd', probs.astype(jnp.float32), near_values.astype(jnp.float32))
        return mixed.astype(jnp.bfloat16).reshape(block, HEADS * HEAD_DIM)
    attended = lax.map(attend, jnp.arange(total // block, dtype=jnp.int32)).reshape(total, HEADS * HEAD_DIM)
    glu = (jnp.dot(normed, w_conv_in, preferred_element_type=jnp.float32) * jax.nn.sigmoid(jnp.dot(normed, w_conv_gate, preferred_element_type=jnp.float32))).astype(jnp.bfloat16)
    reach = TAPS // 2
    padded_glu = jnp.pad(glu.astype(jnp.float32), ((reach, reach), (0, 0)))
    filtered = jnp.zeros((total, CHANNELS), jnp.float32) + conv_bias[None, :]
    for offset in range(TAPS):
        filtered = filtered + conv_taps[offset][None, :] * padded_glu[offset:offset + total]
    centre = lax.optimization_barrier(jnp.mean(filtered, axis=-1, keepdims=True))
    centred = filtered - centre
    spread = lax.optimization_barrier(jnp.mean(centred * centred, axis=-1, keepdims=True))
    conv_out = jax.nn.silu(centred * lax.rsqrt(spread + EPSILON) * channel_gain[None, :] + channel_shift[None, :]).astype(jnp.bfloat16)
    result = jnp.dot(attended, w_attn_out, preferred_element_type=jnp.float32) + jnp.dot(conv_out, w_conv_out, preferred_element_type=jnp.float32)
    return result.astype(jnp.bfloat16)
```

```python
import jax
import jax.numpy as jnp
from jax import lax
from jax.sharding import PartitionSpec as P

HEAD_DIM = 64
KV_GROUP = 4
WINDOW = 128
GRID_W = 64


EPSILON = 1e-06
NEGATIVE = -1e30
ROPE_BASE = 10000.0
F32 = jnp.float32
BF16 = jnp.bfloat16


def rotate_pairs(values, positions):
    middle = values.shape[-1] // 2
    inverse = ROPE_BASE ** (-jnp.arange(middle, dtype=F32) / middle)
    angles = positions.astype(F32)[:, None] * inverse[None, :]
    cosine = jnp.cos(angles)[:, None, :]
    sine_table = jnp.sin(angles)[:, None, :]
    leading = values[..., :middle]
    trailing = values[..., middle:]
    return jnp.concatenate(
        [leading * cosine - trailing * sine_table, leading * sine_table + trailing * cosine],
        axis=-1,
    )


def grid_rotate(values, positions):
    middle = values.shape[-1] // 2
    return jnp.concatenate(
        [
            rotate_pairs(values[..., :middle], positions // GRID_W),
            rotate_pairs(values[..., middle:], positions % GRID_W),
        ],
        axis=-1,
    )


def cut(array, start, size, axis):
    return lax.dynamic_slice_in_dim(array, start, size, axis)


def dot(left, right):
    return jnp.dot(left, right, preferred_element_type=F32)


def local(
    tokens,
    norm_gain,
    w_query,
    w_key,
    w_value,
    w_conv_in,
    w_conv_gate,
    sink_logit,
    conv_taps,
    conv_bias,
    channel_gain,
    channel_shift,
    w_attn_out,
    w_conv_out,
):
    sp, fs, tp = (lax.axis_size(a) for a in ("sp", "fs", "tp"))
    s, f, t = (lax.axis_index(a) for a in ("sp", "fs", "tp"))
    width = tokens.shape[1]
    rows = tokens.shape[0] // tp
    depth = width // sp
    head_cols = w_query.shape[1]
    kv_cols = w_key.shape[1]
    heads = head_cols * tp // HEAD_DIM // fs
    q_cols = heads * HEAD_DIM
    kv_here = max(1, heads // KV_GROUP)
    k_cols = kv_here * HEAD_DIM
    group = heads // kv_here
    chan_half = w_conv_in.shape[1] // fs
    chans = chan_half * tp
    reach = conv_taps.shape[0] // 2

    ring = [(i, (i + 1) % sp) for i in range(sp)]
    swap = [(i, tp - 1 - i) for i in range(tp)]
    chain_up = [(i, i + 1) for i in range(sp * tp - 1)]
    chain_down = [(b, a) for a, b in chain_up]

    def onward(x):
        return lax.ppermute(x, "sp", ring)

    def partner(x):
        return lax.ppermute(x, "tp", swap)

    def across(x, step):
        return lax.ppermute(x, "fs", [(i, i ^ step) for i in range(fs)])

    conv_piece = jnp.concatenate(
        [cut(w_conv_in, f * chan_half, chan_half, 1), cut(w_conv_gate, f * chan_half, chan_half, 1)],
        axis=1,
    )
    q_at = f * q_cols
    kv_at = (f * heads // KV_GROUP) * HEAD_DIM
    qkv_piece = jnp.concatenate(
        [
            cut(w_query, q_at % head_cols, q_cols, 1),
            cut(w_key, kv_at % kv_cols, k_cols, 1),
            cut(w_value, kv_at % kv_cols, k_cols, 1),
        ],
        axis=1,
    )
    half = depth // tp
    qkv_other = partner(cut(qkv_piece, (1 - t) * half, half, 0))
    qkv_piece = jnp.where(q_at // head_cols == t, cut(qkv_piece, t * half, half, 0), qkv_other)

    token_float = cut(tokens, t * rows, rows, 0).astype(F32)
    scale = lax.rsqrt(jnp.mean(token_float * token_float, axis=-1, keepdims=True) + EPSILON)
    normed = (token_float * scale * norm_gain[None, :]).astype(BF16)
    normed = jnp.concatenate([cut(normed, ((s - k) % sp) * depth, depth, 1) for k in range(sp)], axis=1)
    gathered = jnp.concatenate([normed] + [across(normed, j) for j in range(1, fs)], axis=0)
    total_rows = fs * rows

    conv_acc = jnp.zeros((total_rows, 4 * chan_half), F32)
    qkv_acc = jnp.zeros((total_rows, q_cols + 2 * k_cols), F32)
    for k in range(sp):
        block = gathered[:, k * depth : (k + 1) * depth]
        conv_other = partner(conv_piece)
        qkv_other = partner(qkv_piece)
        conv_acc = conv_acc + dot(block, jnp.concatenate([conv_piece, conv_other], axis=1))
        mine = cut(block, t * half, half, 1)
        other = cut(block, (1 - t) * half, half, 1)
        qkv_acc = qkv_acc + dot(mine, qkv_piece) + dot(other, qkv_other)
        if k + 1 < sp:
            conv_piece = onward(conv_piece)
            qkv_piece = onward(qkv_piece)

    attn_half = q_cols // tp
    out_piece = jnp.concatenate(
        [
            cut(w_attn_out, q_at + t * attn_half, attn_half, 0),
            cut(w_conv_out, t * w_conv_in.shape[1] + f * chan_half, chan_half, 0),
        ],
        axis=0,
    )
    out_blocks = []
    for k in range(sp):
        out_blocks.append(jnp.concatenate([out_piece, partner(out_piece)], axis=0))
        if k + 1 < sp:
            out_piece = onward(out_piece)

    c2 = 2 * chan_half
    signal = jnp.concatenate([conv_acc[:, :chan_half], conv_acc[:, c2 : c2 + chan_half]], axis=1)
    gate = jnp.concatenate([conv_acc[:, chan_half:c2], conv_acc[:, c2 + chan_half :]], axis=1)
    glu = (signal * jax.nn.sigmoid(gate)).astype(BF16).reshape(fs, rows, chans)

    def chain(x, pairs):
        return lax.ppermute(x, ("sp", "tp"), pairs)

    def other_order(x):
        return jnp.concatenate([x[..., chan_half:], x[..., :chan_half]], axis=-1)

    low = other_order(chain(glu[:, rows - reach :], chain_up))
    high = other_order(chain(glu[:, :reach], chain_down))
    rims = jnp.concatenate([low, glu, high], axis=1).astype(F32)

    def channel(x):
        both = [cut(x, f * chan_half, chan_half, -1)]
        return jnp.concatenate(both + [partner(both[0])], axis=-1)

    vectors = channel(
        jnp.concatenate(
            [conv_taps, conv_bias[None], channel_gain[None], channel_shift[None]], axis=0
        )
    )
    taps = vectors[: 2 * reach + 1]
    bias, gain, shift = (vectors[2 * reach + 1 + i] for i in range(3))
    filtered = jnp.zeros((fs, rows, chans), F32) + bias
    for k in range(2 * reach + 1):
        filtered = filtered + taps[k] * rims[:, k : k + rows]
    own_mean = jnp.sum(filtered, axis=-1) / chans
    own_square = jnp.sum((filtered - own_mean[..., None]) ** 2, axis=-1)
    stats = jnp.stack([own_mean, own_square])
    everyone = [stats]
    for j in range(1, fs):
        there = across(stats, j)
        everyone.append(jnp.stack([there[:, i ^ j] for i in range(fs)], axis=1))
    everyone = jnp.stack(everyone)
    centre = jnp.mean(everyone[:, 0], axis=0)
    spread = (
        jnp.sum(everyone[:, 1], axis=0) + chans * jnp.sum((everyone[:, 0] - centre) ** 2, axis=0)
    ) / (chans * fs)
    conv_out = jax.nn.silu(
        (filtered - centre[..., None]) * lax.rsqrt(spread + EPSILON)[..., None] * gain + shift
    ).astype(BF16).reshape(total_rows, chans)

    start = (s * tp + t) * rows
    positions = start + jnp.arange(rows, dtype=jnp.int32)
    positions_all = jnp.tile(positions, fs)
    query = grid_rotate(qkv_acc[:, :q_cols].reshape(total_rows, heads, HEAD_DIM), positions_all)
    query = query.astype(BF16).reshape(fs, rows, kv_here, group, HEAD_DIM)
    keys = grid_rotate(
        qkv_acc[:, q_cols : q_cols + k_cols].reshape(total_rows, kv_here, HEAD_DIM), positions_all
    ).astype(BF16).reshape(total_rows, k_cols)
    values = qkv_acc[:, q_cols + k_cols :].astype(BF16)
    stacked = jnp.concatenate([keys, values], axis=1).reshape(fs, rows, 2 * k_cols)
    below = chain(stacked[:, rows - WINDOW :], chain_up)
    above = chain(stacked[:, :WINDOW], chain_down)
    extended = jnp.concatenate([below, stacked, above], axis=1)
    span = rows + 2 * WINDOW
    near_keys = extended[..., :k_cols].reshape(fs, span, kv_here, HEAD_DIM)
    near_values = extended[..., k_cols:].reshape(fs, span, kv_here, HEAD_DIM)
    sink_mine = cut(sink_logit, (f * heads) % sink_logit.shape[0], heads, 0)
    sinks = jnp.where(q_at // head_cols == t, sink_mine, partner(sink_mine))
    sinks = sinks.reshape(kv_here, group)[None, :, :, None, None]
    scores = jnp.einsum(
        "fqkgd,fskd->fkgqs", query, near_keys, preferred_element_type=F32
    ) * HEAD_DIM ** (-0.5)
    key_pos = start - WINDOW + jnp.arange(span, dtype=jnp.int32)
    valid = (
        (jnp.abs(positions[:, None] - key_pos[None, :]) <= WINDOW)
        & (key_pos[None, :] >= 0)
        & (key_pos[None, :] < rows * sp * tp)
    )
    scores = jnp.where(valid, scores, NEGATIVE)
    top = jnp.maximum(jnp.max(scores, axis=-1, keepdims=True), sinks)
    raised = jnp.exp(scores - top)
    denominator = jnp.sum(raised, axis=-1, keepdims=True) + jnp.exp(sinks - top)
    probs = (raised / denominator).astype(BF16)
    mixed = jnp.einsum("fkgqs,fskd->fqkgd", probs, near_values, preferred_element_type=F32)
    attended = mixed.astype(BF16).reshape(total_rows, q_cols)

    features = jnp.concatenate(
        [
            cut(attended, t * attn_half, attn_half, 1),
            conv_out[:, :chan_half],
            cut(attended, (1 - t) * attn_half, attn_half, 1),
            conv_out[:, chan_half:],
        ],
        axis=1,
    )
    partial = jnp.concatenate([dot(features, w) for w in out_blocks], axis=1)
    partial = partial.reshape(fs, rows, width)
    result = partial[0]
    for j in range(1, fs):
        result = result + across(partial[j].astype(BF16), j).astype(F32)
    result = result.astype(BF16)
    return jnp.concatenate([cut(result, ((s - k) % sp) * depth, depth, 1) for k in range(sp)], axis=1)


def solution(mesh):
    in_specs = (
        P(("fs", "sp"), None),
        P(),
        P("sp", "tp"),
        P("sp", "tp"),
        P("sp", "tp"),
        P("sp", "tp"),
        P("sp", "tp"),
        P("tp"),
        P(None, "tp"),
        P("tp"),
        P("tp"),
        P("tp"),
        P(None, "sp"),
        P(None, "sp"),
    )
    out_specs = P(("fs", "sp", "tp"), None)
    return jax.shard_map(local, mesh=mesh, in_specs=in_specs, out_specs=out_specs, check_vma=False)
```
